32 devices in a mesh: grp: 2 (over y), fs: 4 (over z), tp: 4 (over x, core).
Axes of the slice: x: 2, y: 2, z: 4, core: 2. Of those that a mesh axis runs over, the one named last changes fastest.
Arguments:
- tokens: bfloat16 [8, 384, 2048], P(('grp', 'fs'), None, 'tp'), parts along dimension 0, may hold values from -24 to 24
- input_gain: float32 [2048], replicated, may hold values from 0.1 to 1.9
- query_weight: bfloat16 [2048, 1024], P('fs', 'tp'), may hold values from -0.125 to 0.125
- key_weight: bfloat16 [2048, 1024], P('fs', 'tp'), may hold values from -0.125 to 0.125
- value_weight: bfloat16 [2048, 1024], P('fs', 'tp'), may hold values from -0.125 to 0.125
- output_gate_matrix: bfloat16 [2048, 1024], P('fs', 'tp'), may hold values from -0.125 to 0.125
- forward_decay: float32 [16], P('tp'), may hold values from -1 to 9
- backward_decay: float32 [16], P('tp'), may hold values from -1 to 9
- merge_weight: bfloat16 [1024, 2048], P('tp', 'fs'), may hold values from -0.375 to 0.375
- middle_gain: float32 [2048], replicated, may hold values from 0.1 to 1.9
- gate_weight: bfloat16 [2048, 5120], P('fs', 'tp'), may hold values from -0.125 to 0.125
- up_weight: bfloat16 [2048, 5120], P('fs', 'tp'), may hold values from -0.125 to 0.125
- down_weight: bfloat16 [5120, 2048], P('tp', 'fs'), may hold values from -0.15625 to 0.15625
Outputs:
- layer_out: bfloat16 [8, 384, 2048], P(('grp', 'fs'), None, 'tp'), parts along dimension 0
The draws below stay inside these ranges and needn't reach their ends.
There are 2 independent parts, one for each index of `grp`. The reference program is written for one: setup_inputs(seed, part) draws one part's arguments, and reference() takes and returns one part's arrays. A program takes and returns all parts, laid end to end along the dimension named above; an argument that names none is the same for every part. Nothing has to cross between parts.
All inputs are finite; a program needn't handle non-finite values.
Results may differ from the reference program's by a relative error of at most 0.019.
Values may be sent and summed in bfloat16 or wider, within the bound.
A program may use at most 64 MiB of HBM per device.

```python
import math
import jax
import jax.numpy as jnp
from jax import lax

D = 2048
HEADS = 16
FF = 5120
BLOCK = 128
LEN = 384
RET_W = 1024
SEQS = 4
N_TP = 4


def draw_tokens(key, part):
    subkeys = jax.random.split(jax.random.fold_in(key, 11), 3)
    full_shape = (SEQS, LEN, D)
    row_scale = jnp.exp(jax.random.uniform(subkeys[1], (SEQS, LEN, 1), jnp.float32, math.log(0.3), math.log(3.0)))
    column_scale = jnp.exp(jax.random.uniform(subkeys[2], (1, 1, D), jnp.float32, math.log(0.5), math.log(2.0)))
    base_values = jnp.clip(jax.random.normal(subkeys[0], full_shape, jnp.float32), -4.0, 4.0)
    return (base_values * row_scale * column_scale).astype(jnp.bfloat16)


def decay_logits(key, salt):
    subkeys = jax.random.split(jax.random.fold_in(key, salt), 3)
    slow_share = 0.5
    slow_low = 0.7
    slow_high = 2.3
    is_slow = jax.random.bernoulli(subkeys[0], slow_share, (HEADS,))
    slow_rate = -jax.random.uniform(subkeys[1], (HEADS,), jnp.float32, slow_low, slow_high) / LEN
    fast_rate = -jax.random.uniform(subkeys[2], (HEADS,), jnp.float32, 7.5, 15.0) / BLOCK
    log_rates = jnp.where(is_slow, slow_rate, fast_rate)
    return log_rates - jnp.log(-jnp.expm1(log_rates))


def draw_forward_decay(key, part):
    return decay_logits(key, 21)


def draw_backward_decay(key, part):
    return decay_logits(key, 22)


def levels(stream_key, dims, pieces, smallest, largest):
    gain, own = 1.0, jax.random.fold_in(stream_key, 6)
    for dim, blocks in pieces:
        draws = jnp.exp(jax.random.uniform(jax.random.fold_in(own, dim), (blocks,), jnp.float32, smallest / len(pieces), largest / len(pieces)))
        gain = gain * jnp.repeat(draws, dims[dim] // blocks).reshape([-1 if axis == dim else 1 for axis in range(len(dims))])
    return gain


def scatter_about(stream_key, shape, scale, bound, cuts=(), kind=jnp.bfloat16):
    level = levels(stream_key, shape, cuts, -0.22, 0.18) if cuts else 1.0
    values = jax.random.normal(stream_key, shape, jnp.float32) * scale * level
    return jnp.minimum(jnp.maximum(values, -bound), bound).astype(kind)


def setup_inputs(seed: int = 0, part: int = 0) -> dict:
    arg_keys = jax.random.split(jax.random.key(seed), 14)
    part_splits = jax.random.split(jax.random.fold_in(arg_keys[13], part), 14)
    return {
        "tokens": draw_tokens(jax.random.fold_in(jax.random.fold_in(arg_keys[13], part), 71), part),
        "input_gain": jnp.clip(1.0 + 0.18 * jax.random.normal(arg_keys[1], (D,), jnp.float32), 0.1, 1.9),
        "query_weight": scatter_about(arg_keys[2], (D, RET_W), D ** -0.5, 0.125, ((0, 4), (1, 4))),
        "key_weight": scatter_about(arg_keys[3], (D, RET_W), D ** -0.5, 0.125, ((0, 4), (1, 4))),
        "value_weight": scatter_about(arg_keys[4], (D, RET_W), D ** -0.5, 0.125, ((0, 4), (1, 4))),
        "output_gate_matrix": scatter_about(arg_keys[5], (D, RET_W), D ** -0.5, 0.125, ((0, 4), (1, 4))),
        "forward_decay": draw_forward_decay(jax.random.fold_in(arg_keys[13], 71), part),
        "backward_decay": draw_backward_decay(jax.random.fold_in(arg_keys[13], 71), part),
        "merge_weight": scatter_about(arg_keys[8], (RET_W, D), (RET_W // 4) ** -0.5, 0.375, ((0, 4), (1, 4))),
        "middle_gain": jnp.clip(1.0 + 0.18 * jax.random.normal(arg_keys[9], (D,), jnp.float32), 0.1, 1.9),
        "gate_weight": scatter_about(arg_keys[10], (D, FF), D ** -0.5, 0.125, ((0, 4), (1, 4))),
        "up_weight": scatter_about(arg_keys[11], (D, FF), D ** -0.5, 0.125, ((0, 4), (1, 4))),
        "down_weight": scatter_about(arg_keys[12], (FF, D), (FF // 4) ** -0.5, 0.15625, ((0, 4), (1, 4))),
    }


norm_eps = 1e-06
group_eps = 1e-05
rope_base = 10000.0
highest_precision = lax.Precision.HIGHEST

def rms_scale(values, gain_vector):
    widened = values.astype(jnp.float32)
    scaled = widened * lax.rsqrt(lax.optimization_barrier(jnp.mean(widened * widened, axis=-1, keepdims=True)) + norm_eps)
    return (scaled * gain_vector.astype(jnp.float32)).astype(jnp.bfloat16)

def apply_rotary_heads(values, length):
    half_dim = values.shape[-1] // 2
    inverse = rope_base ** (-jnp.arange(half_dim, dtype=jnp.float32) / half_dim)
    angles = jnp.arange(length, dtype=jnp.float32)[:, None] * inverse[None, :]
    cosine = jnp.cos(angles)[:, None, :]
    sine_part = jnp.sin(angles)[:, None, :]
    lower_half = values[..., :half_dim]
    upper_half = values[..., half_dim:]
    return jnp.concatenate([lower_half * cosine - upper_half * sine_part, upper_half * cosine + lower_half * sine_part], axis=-1)

def retain_dense(query_rows, key_rows, value_rows, gate_rows, forward_decay, backward_decay, seq_count, length):
    head_count = forward_decay.shape[0]
    head_dim = query_rows.shape[1] // head_count

    def split_heads(rows_in):
        return rows_in.astype(jnp.float32).reshape(seq_count, length, head_count, head_dim)
    queries = apply_rotary_heads(split_heads(query_rows), length)
    key_heads = apply_rotary_heads(split_heads(key_rows), length) * head_dim ** (-0.5)
    valued = split_heads(value_rows)
    rate_ahead = jax.nn.log_sigmoid(forward_decay.astype(jnp.float32))
    rate_behind = jax.nn.log_sigmoid(backward_decay.astype(jnp.float32))
    position = jnp.arange(length, dtype=jnp.float32)
    offset = position[:, None] - position[None, :]
    weight_tree = jnp.where(offset[None] >= 0, jnp.exp(rate_ahead[:, None, None] * jnp.maximum(offset, 0.0)[None]), jnp.exp(rate_behind[:, None, None] * jnp.maximum(-offset, 0.0)[None]))

    def one_sequence(operands):
        sequence_query, sequence_key, sequence_value = operands
        attention_scores = jnp.einsum('pze,rze->zpr', sequence_query, sequence_key, precision=highest_precision) * weight_tree
        return jnp.einsum('kaf,fkg->akg', attention_scores, sequence_value, precision=highest_precision)
    result = lax.map(one_sequence, (queries, key_heads, valued))
    center = lax.optimization_barrier(jnp.mean(result, axis=-1, keepdims=True))
    spread = lax.optimization_barrier(jnp.mean(jnp.square(result - center), axis=-1, keepdims=True))
    normalized = (result - center) * lax.rsqrt(spread + group_eps)
    gated = jax.nn.silu(split_heads(gate_rows)) * normalized
    return gated.reshape(seq_count * length, head_count * head_dim).astype(jnp.bfloat16)

def split_sum(left_rows, right_rows):
    group_size = left_rows.shape[1] // N_TP
    total = jnp.zeros((left_rows.shape[0], right_rows.shape[1]), jnp.float32)
    for index in range(N_TP):
        lower = index * group_size
        partial_term = jnp.dot(left_rows[:, lower:lower + group_size], right_rows[lower:lower + group_size], preferred_element_type=jnp.float32).astype(jnp.bfloat16)
        total = total + lax.optimization_barrier(partial_term).astype(jnp.float32)
    return total

def reference(tokens, input_gain, query_weight, key_weight, value_weight, output_gate_matrix, forward_decay, backward_decay, merge_weight, middle_gain, gate_weight, up_weight, down_weight):
    seq_count, length, width = tokens.shape
    row_count = seq_count * length
    flat = tokens.reshape(row_count, width)
    normed = rms_scale(flat, input_gain)
    query_rows = jnp.dot(normed, query_weight, preferred_element_type=jnp.float32).astype(jnp.bfloat16)
    key_rows = jnp.dot(normed, key_weight, preferred_element_type=jnp.float32).astype(jnp.bfloat16)
    value_rows = jnp.dot(normed, value_weight, preferred_element_type=jnp.float32).astype(jnp.bfloat16)
    gate_rows = jnp.dot(normed, output_gate_matrix, preferred_element_type=jnp.float32).astype(jnp.bfloat16)
    mixed = retain_dense(query_rows, key_rows, value_rows, gate_rows, forward_decay, backward_decay, seq_count, length)
    middle = (flat.astype(jnp.float32) + split_sum(mixed, merge_weight)).astype(jnp.bfloat16)
    normed_mid = rms_scale(middle, middle_gain)
    gate_act = jnp.dot(normed_mid, gate_weight, preferred_element_type=jnp.float32)
    up_act = jnp.dot(normed_mid, up_weight, preferred_element_type=jnp.float32)
    hidden = (jax.nn.silu(gate_act) * up_act).astype(jnp.bfloat16)
    layer_out = (middle.astype(jnp.float32) + split_sum(hidden, down_weight)).astype(jnp.bfloat16)
    return layer_out.reshape(seq_count, length, width)
```

```python
import functools

import jax
import jax.numpy as jnp
from jax import lax
from jax.experimental import pallas as pl
from jax.experimental.pallas import tpu as pltpu
from jax.sharding import PartitionSpec as P

BLOCK = 128


norm_eps = 1e-06
group_eps = 1e-05
rope_base = 10000.0
highest_precision = lax.Precision.HIGHEST


def rms_scale(values, gain_vector):
    widened = values.astype(jnp.float32)
    scaled = widened * lax.rsqrt(jnp.mean(widened * widened, axis=-1, keepdims=True) + norm_eps)
    return (scaled * gain_vector).astype(jnp.bfloat16)


def apply_rotary_heads(values, length):
    half_dim = values.shape[-1] // 2
    inverse = rope_base ** (-jnp.arange(half_dim, dtype=jnp.float32) / half_dim)
    angles = jnp.arange(length, dtype=jnp.float32)[:, None] * inverse[None, :]
    cosine = jnp.cos(angles)[:, None, :]
    sine_part = jnp.sin(angles)[:, None, :]
    lower_half = values[..., :half_dim]
    upper_half = values[..., half_dim:]
    return jnp.concatenate(
        [
            lower_half * cosine - upper_half * sine_part,
            upper_half * cosine + lower_half * sine_part,
        ],
        axis=-1,
    )


def carry_states(key_blocks, value_blocks, weighting, log_rates, block_size, backward):
    block_terms = jnp.einsum(
        "sbmhd,sbmhe->bshde",
        key_blocks * weighting[None, None, :, :, None],
        value_blocks,
        precision=highest_precision,
    )
    factor = jnp.exp(log_rates * block_size)[None, :, None, None]

    def advance(running, addend):
        return (running * factor + addend, running)

    initial = jnp.zeros(block_terms.shape[1:], jnp.float32)
    return lax.scan(advance, initial, block_terms, reverse=backward)[1]


def retain_blocks(
    query_rows, key_rows, value_rows, gate_rows, forward_decay, backward_decay, seq_count, length
):
    head_count = forward_decay.shape[0]
    head_dim = query_rows.shape[1] // head_count
    block_size = BLOCK
    block_count = length // block_size

    def split_heads(rows_in):
        return rows_in.astype(jnp.float32).reshape(seq_count, length, head_count, head_dim)

    def blocked(tensor):
        return tensor.reshape(seq_count, block_count, block_size, head_count, head_dim)

    queries = blocked(apply_rotary_heads(split_heads(query_rows), length))
    key_heads = blocked(apply_rotary_heads(split_heads(key_rows), length) * head_dim ** (-0.5))
    valued = blocked(split_heads(value_rows))
    rate_ahead = jax.nn.log_sigmoid(forward_decay)
    rate_behind = jax.nn.log_sigmoid(backward_decay)
    position = jnp.arange(block_size, dtype=jnp.float32)
    offset = position[:, None] - position[None, :]
    inside = jnp.where(
        offset[None] >= 0,
        jnp.exp(rate_ahead[:, None, None] * jnp.maximum(offset, 0.0)[None]),
        jnp.exp(rate_behind[:, None, None] * jnp.maximum(-offset, 0.0)[None]),
    )
    attention_scores = (
        jnp.einsum("sbchd,sbmhd->sbhcm", queries, key_heads, precision=highest_precision)
        * inside[None, None]
    )
    result = jnp.einsum("sbhcm,sbmhd->sbchd", attention_scores, valued, precision=highest_precision)
    column = position[:, None]
    key_ahead = jnp.exp(rate_ahead[None, :] * (block_size - 1 - column))
    query_ahead = jnp.exp(rate_ahead[None, :] * (column + 1))
    key_behind = jnp.exp(rate_behind[None, :] * column)
    query_behind = jnp.exp(rate_behind[None, :] * (block_size - column))
    from_before = carry_states(key_heads, valued, key_ahead, rate_ahead, block_size, False)
    from_after = carry_states(key_heads, valued, key_behind, rate_behind, block_size, True)
    result = (
        result
        + jnp.einsum("sbchd,bshde->sbche", queries, from_before, precision=highest_precision)
        * query_ahead[None, None, :, :, None]
    )
    result = (
        result
        + jnp.einsum("sbchd,bshde->sbche", queries, from_after, precision=highest_precision)
        * query_behind[None, None, :, :, None]
    )
    result = result.reshape(seq_count, length, head_count, head_dim)
    center = jnp.mean(result, axis=-1, keepdims=True)
    spread = jnp.mean(jnp.square(result - center), axis=-1, keepdims=True)
    normalized = (result - center) * lax.rsqrt(spread + group_eps)
    gated = jax.nn.silu(split_heads(gate_rows)) * normalized
    return gated.reshape(seq_count * length, head_count * head_dim).astype(jnp.bfloat16)


MESH = pl.DeviceIdType.MESH


def gather_kernel(sizes, *refs):
    line, copies = sizes["fs"], sizes["grp"]
    count = len(refs[:-5]) // 2
    shards, slots = refs[:count], refs[count : 2 * count]
    own_sem, line_send, line_recv, pair_send, pair_recv = refs[2 * count :]
    place = lax.axis_index("fs")
    half = lax.axis_index("grp")

    barrier = pltpu.get_barrier_semaphore()
    for shift in (1, -1):
        there = place + shift

        @pl.when((there >= 0) & (there < line))
        def _():
            pl.semaphore_signal(barrier, inc=1, device_id={"fs": there}, device_id_type=MESH)

    for other in range(1, copies):
        pl.semaphore_signal(
            barrier,
            inc=1,
            device_id={"grp": lax.rem(half + other, copies)},
            device_id_type=MESH,
        )
    own = [pltpu.make_async_copy(shards[k], slots[k].at[place], own_sem.at[k]) for k in range(count)]
    for copy in own:
        copy.start()
    neighbours = (place > 0).astype(jnp.int32) + (place < line - 1).astype(jnp.int32)
    pl.semaphore_wait(barrier, neighbours + copies - 1)

    def piece(k, block, part):
        rows = slots[k].shape[1] // copies
        return slots[k].at[block, pl.ds(pl.multiple_of(part * rows, rows), rows), :]

    def hop(k, way, step):
        shift = 1 if way == 0 else -1
        block = place - shift * step
        return pltpu.make_async_remote_copy(
            src_ref=piece(k, block, half),
            dst_ref=piece(k, block, half),
            send_sem=line_send.at[k, way, step],
            recv_sem=line_recv.at[k, way, step],
            device_id={"fs": place + shift},
            device_id_type=MESH,
        )

    def arrival(k, way, step):
        shift = 1 if way == 0 else -1
        block = place - shift * step
        return pltpu.make_async_remote_copy(
            src_ref=piece(k, block, half),
            dst_ref=piece(k, block, half),
            send_sem=line_send.at[k, way, step - 1],
            recv_sem=line_recv.at[k, way, step - 1],
            device_id={"fs": place - shift},
            device_id_type=MESH,
        )

    def across(k, way, step, other):
        shift = 1 if way == 0 else -1
        block = place - shift * step
        return pltpu.make_async_remote_copy(
            src_ref=piece(k, block, half),
            dst_ref=piece(k, block, half),
            send_sem=pair_send.at[k, way, step - 1, other - 1],
            recv_sem=pair_recv.at[k, way, step - 1, other - 1],
            device_id={"grp": lax.rem(half + other, copies)},
            device_id_type=MESH,
        )

    def landed(k, way, step, other):
        shift = 1 if way == 0 else -1
        block = place - shift * step
        source = lax.rem(half + copies - other, copies)
        return pltpu.make_async_remote_copy(
            src_ref=piece(k, block, source),
            dst_ref=piece(k, block, source),
            send_sem=pair_send.at[k, way, step - 1, other - 1],
            recv_sem=pair_recv.at[k, way, step - 1, other - 1],
            device_id={"grp": source},
            device_id_type=MESH,
        )

    def has(way, step):
        return place >= step if way == 0 else place + step < line

    def goes(way):
        return place < line - 1 if way == 0 else place > 0

    def launch(k):
        own[k].wait()
        for way in range(2):

            @pl.when(goes(way))
            def _():
                hop(k, way, 0).start()

    def pump(k):
        for step in range(1, line):
            for way in range(2):

                @pl.when(has(way, step))
                def _():
                    arrival(k, way, step).wait_recv()
                    for other in range(1, copies):
                        across(k, way, step, other).start()

                @pl.when(has(way, step) & goes(way))
                def _():
                    hop(k, way, step).start()

    def settle(k):
        for step in range(1, line):
            for way in range(2):

                @pl.when(has(way, step))
                def _():
                    for other in range(1, copies):
                        landed(k, way, step, other).wait_recv()

    def drain(k):
        for way in range(2):
            for step in range(line):

                @pl.when((has(way, step) if step else True) & goes(way))
                def _():
                    hop(k, way, step).wait_send()

                if step:

                    @pl.when(has(way, step))
                    def _():
                        for other in range(1, copies):
                            across(k, way, step, other).wait_send()

    for k in range(min(2, count)):
        launch(k)
    for k in range(count):
        pump(k)
        if k + 2 < count:
            launch(k + 2)
    for k in range(count):
        settle(k)
        drain(k)


def gather_weights(sizes, shards):
    line, copies, count = sizes["fs"], sizes["grp"], len(shards)
    return pl.pallas_call(
        functools.partial(gather_kernel, sizes),
        out_shape=[jax.ShapeDtypeStruct((line,) + w.shape, w.dtype) for w in shards],
        in_specs=[pl.BlockSpec(memory_space=pl.ANY)] * count,
        out_specs=[pl.BlockSpec(memory_space=pltpu.VMEM)] * count,
        scratch_shapes=[
            pltpu.SemaphoreType.DMA((count,)),
            pltpu.SemaphoreType.DMA((count, 2, line)),
            pltpu.SemaphoreType.DMA((count, 2, line)),
            pltpu.SemaphoreType.DMA((count, 2, line, copies - 1)),
            pltpu.SemaphoreType.DMA((count, 2, line, copies - 1)),
        ],
        compiler_params=pltpu.CompilerParams(
            collective_id=0, has_side_effects=True, vmem_limit_bytes=56 << 20
        ),
    )(*shards)


def rows_of(blocks):
    return blocks.reshape(-1, blocks.shape[2])


def columns_of(blocks):
    return blocks.transpose(1, 0, 2).reshape(blocks.shape[1], -1)


def on_device(
    sizes,
    tokens,
    input_gain,
    query_weight,
    key_weight,
    value_weight,
    output_gate_matrix,
    forward_decay,
    backward_decay,
    merge_weight,
    middle_gain,
    gate_weight,
    up_weight,
    down_weight,
):
    seq_count, length, part_width = tokens.shape
    row_count = seq_count * length
    joined = jnp.concatenate([query_weight, key_weight, value_weight, output_gate_matrix], axis=1)
    joined_full, merge_full, gate_full, up_full, down_full = gather_weights(
        sizes, (joined, merge_weight, gate_weight, up_weight, down_weight)
    )
    merge_full, down_full = columns_of(merge_full), columns_of(down_full)
    gate_full, up_full = rows_of(gate_full), rows_of(up_full)
    gathered = lax.all_gather(tokens, "tp", axis=2, tiled=True)
    normed = rms_scale(gathered.reshape(row_count, gathered.shape[2]), input_gain)
    projected = jnp.dot(normed, rows_of(joined_full), preferred_element_type=jnp.float32)
    query_sum, key_sum, value_sum, gating_sum = jnp.split(projected, 4, axis=1)
    mixed = retain_blocks(
        query_sum.astype(jnp.bfloat16),
        key_sum.astype(jnp.bfloat16),
        value_sum.astype(jnp.bfloat16),
        gating_sum.astype(jnp.bfloat16),
        forward_decay,
        backward_decay,
        seq_count,
        length,
    )
    merge_term = jnp.dot(
        mixed,
        merge_full,
        preferred_element_type=jnp.float32,
    )
    merged = lax.psum_scatter(
        merge_term.astype(jnp.bfloat16), "tp", scatter_dimension=1, tiled=True
    ).astype(jnp.float32)
    middle = (tokens.reshape(row_count, part_width).astype(jnp.float32) + merged).astype(
        jnp.bfloat16
    )
    gathered_mid = lax.all_gather(middle, "tp", axis=1, tiled=True)
    normed_mid = rms_scale(gathered_mid, middle_gain)
    gate_act = jnp.dot(normed_mid, gate_full, preferred_element_type=jnp.float32)
    up_act = jnp.dot(normed_mid, up_full, preferred_element_type=jnp.float32)
    hidden = (jax.nn.silu(gate_act) * up_act).astype(jnp.bfloat16)
    down_term = jnp.dot(
        hidden,
        down_full,
        preferred_element_type=jnp.float32,
    )
    summed = lax.psum_scatter(
        down_term.astype(jnp.bfloat16), "tp", scatter_dimension=1, tiled=True
    ).astype(jnp.float32)
    layer_out = (middle.astype(jnp.float32) + summed).astype(jnp.bfloat16)
    return layer_out.reshape(seq_count, length, part_width)


def solution(mesh):
    placed = (
        P(("grp", "fs"), None, "tp"),
        P(),
        P("fs", "tp"),
        P("fs", "tp"),
        P("fs", "tp"),
        P("fs", "tp"),
        P("tp"),
        P("tp"),
        P("tp", "fs"),
        P(),
        P("fs", "tp"),
        P("fs", "tp"),
        P("tp", "fs"),
    )
    return jax.shard_map(
        functools.partial(on_device, dict(mesh.shape)),
        mesh=mesh,
        in_specs=placed,
        out_specs=P(("grp", "fs"), None, "tp"),
        check_vma=False,
    )
```

```python
import functools

import jax
import jax.numpy as jnp
from jax import lax
from jax.experimental import pallas as pl
from jax.experimental.pallas import tpu as pltpu
from jax.sharding import PartitionSpec as P

norm_eps = 1e-06
group_eps = 1e-05
rope_base = 10000.0


def turn_tables(length, head_dim, head_count):
    half_dim = head_dim // 2
    inverse = rope_base ** (-jnp.arange(half_dim, dtype=jnp.float32) / half_dim)
    angles = jnp.arange(length, dtype=jnp.float32)[:, None] * inverse[None, :]
    cosine, sine_part = jnp.cos(angles), jnp.sin(angles)
    return (
        jnp.tile(jnp.concatenate([cosine, cosine], axis=1), (1, head_count)),
        jnp.tile(jnp.concatenate([-sine_part, sine_part], axis=1), (1, head_count)),
    )


MESH = pl.DeviceIdType.MESH


def layer_kernel(
    sizes,
    tokens,
    input_gain,
    middle_gain,
    rate_ahead,
    rate_behind,
    cosine,
    sine_part,
    joined_shard,
    merge_shard,
    gate_shard,
    up_shard,
    down_shard,
    out,
    joined,
    merge,
    gate,
    up,
    down,
    gathered,
    gathered_mid,
    normed,
    projected,
    mixed,
    hidden,
    partial,
    received,
    partial_end,
    received_end,
    own_sem,
    line_send,
    line_recv,
    pair_send,
    pair_recv,
    row_send,
    row_recv,
    self_sem,
):
    line, copies, row = sizes["fs"], sizes["grp"], sizes["tp"]
    shards = (joined_shard, merge_shard, gate_shard, up_shard, down_shard)
    slots = (joined, merge, gate, up, down)
    count = len(slots)
    length, part_width = tokens.shape
    width = row * part_width
    seat = lax.axis_index("tp")
    place = lax.axis_index("fs")
    half = lax.axis_index("grp")

    barrier = pltpu.get_barrier_semaphore()
    for shift in (1, -1):
        there = place + shift

        @pl.when((there >= 0) & (there < line))
        def _():
            pl.semaphore_signal(barrier, inc=1, device_id={"fs": there}, device_id_type=MESH)

    for other in range(1, copies):
        pl.semaphore_signal(
            barrier,
            inc=1,
            device_id={"grp": lax.rem(half + other, copies)},
            device_id_type=MESH,
        )
    for other in range(1, row):
        pl.semaphore_signal(
            barrier,
            inc=1,
            device_id={"tp": lax.rem(seat + other, row)},
            device_id_type=MESH,
        )
    own = [pltpu.make_async_copy(shards[k], slots[k].at[place], own_sem.at[k]) for k in range(count)]
    for copy in own:
        copy.start()
    neighbours = (place > 0).astype(jnp.int32) + (place < line - 1).astype(jnp.int32)
    mine = pltpu.make_async_copy(tokens, gathered.at[seat], self_sem)
    mine.start()
    pl.semaphore_wait(barrier, neighbours + copies - 1 + row - 1)

    def piece(k, block, part):
        rows = slots[k].shape[1] // copies
        return slots[k].at[block, pl.ds(pl.multiple_of(part * rows, rows), rows), :]

    def hop(k, way, step):
        shift = 1 if way == 0 else -1
        block = place - shift * step
        return pltpu.make_async_remote_copy(
            src_ref=piece(k, block, half),
            dst_ref=piece(k, block, half),
            send_sem=line_send.at[k, way, step],
            recv_sem=line_recv.at[k, way, step],
            device_id={"fs": place + shift},
            device_id_type=MESH,
        )

    def arrival(k, way, step):
        shift = 1 if way == 0 else -1
        block = place - shift * step
        return pltpu.make_async_remote_copy(
            src_ref=piece(k, block, half),
            dst_ref=piece(k, block, half),
            send_sem=line_send.at[k, way, step - 1],
            recv_sem=line_recv.at[k, way, step - 1],
            device_id={"fs": place - shift},
            device_id_type=MESH,
        )

    def across(k, way, step, other):
        shift = 1 if way == 0 else -1
        block = place - shift * step
        return pltpu.make_async_remote_copy(
            src_ref=piece(k, block, half),
            dst_ref=piece(k, block, half),
            send_sem=pair_send.at[k, way, step - 1, other - 1],
            recv_sem=pair_recv.at[k, way, step - 1, other - 1],
            device_id={"grp": lax.rem(half + other, copies)},
            device_id_type=MESH,
        )

    def landed(k, way, step, other):
        shift = 1 if way == 0 else -1
        block = place - shift * step
        source = lax.rem(half + copies - other, copies)
        return pltpu.make_async_remote_copy(
            src_ref=piece(k, block, source),
            dst_ref=piece(k, block, source),
            send_sem=pair_send.at[k, way, step - 1, other - 1],
            recv_sem=pair_recv.at[k, way, step - 1, other - 1],
            device_id={"grp": source},
            device_id_type=MESH,
        )

    def has(way, step):
        return place >= step if way == 0 else place + step < line

    def goes(way):
        return place < line - 1 if way == 0 else place > 0

    def launch(k):
        own[k].wait()
        for way in range(2):

            @pl.when(goes(way))
            def _():
                hop(k, way, 0).start()

    def pump(k):
        for step in range(1, line):
            for way in range(2):

                @pl.when(has(way, step))
                def _():
                    arrival(k, way, step).wait_recv()
                    for other in range(1, copies):
                        across(k, way, step, other).start()

                @pl.when(has(way, step) & goes(way))
                def _():
                    hop(k, way, step).start()

    def settle(k):
        for step in range(1, line):
            for way in range(2):

                @pl.when(has(way, step))
                def _():
                    for other in range(1, copies):
                        landed(k, way, step, other).wait_recv()

    def drain(k):
        for way in range(2):
            for step in range(line):

                @pl.when((has(way, step) if step else True) & goes(way))
                def _():
                    hop(k, way, step).wait_send()

                if step:

                    @pl.when(has(way, step))
                    def _():
                        for other in range(1, copies):
                            across(k, way, step, other).wait_send()

    def spread(source, target, stage):
        return [
            pltpu.make_async_remote_copy(
                src_ref=source,
                dst_ref=target.at[seat],
                send_sem=row_send.at[stage, other - 1],
                recv_sem=row_recv.at[stage, other - 1],
                device_id={"tp": lax.rem(seat + other, row)},
                device_id_type=MESH,
            )
            for other in range(1, row)
        ]

    def spread_in(target, stage):
        sources = [lax.rem(seat + row - other, row) for other in range(1, row)]
        return [
            pltpu.make_async_remote_copy(
                src_ref=target.at[source],
                dst_ref=target.at[source],
                send_sem=row_send.at[stage, other],
                recv_sem=row_recv.at[stage, other],
                device_id={"tp": source},
                device_id_type=MESH,
            )
            for other, source in enumerate(sources)
        ]

    def scatter(source, target, stage, other):
        there = lax.rem(seat + other, row)
        return pltpu.make_async_remote_copy(
            src_ref=source.at[there],
            dst_ref=target.at[other - 1],
            send_sem=row_send.at[stage, other - 1],
            recv_sem=row_recv.at[stage, other - 1],
            device_id={"tp": there},
            device_id_type=MESH,
        )

    def normalize(source, gain_vector):
        total = jnp.zeros((length, 1), jnp.float32)
        for t in range(row):
            widened = source[t].astype(jnp.float32)
            total = total + jnp.sum(widened * widened, axis=1, keepdims=True)
        scale = lax.rsqrt(total / width + norm_eps)
        for t in range(row):
            span = slice(t * part_width, (t + 1) * part_width)
            scaled = source[t].astype(jnp.float32) * scale * gain_vector[:, span]
            normed[:, span] = scaled.astype(jnp.bfloat16)

    def times(weight, columns):
        block = weight[:, :, columns]
        return jnp.dot(
            normed[...], block.reshape(-1, block.shape[2]), preferred_element_type=jnp.float32
        )

    def shares(rows_in, weight, target):
        step = weight.shape[2]
        for block in range(line):
            term = jnp.dot(rows_in[...], weight[block], preferred_element_type=jnp.float32)
            begin = block * step
            inner = begin % part_width
            target[begin // part_width, :, inner : inner + step] = term.astype(jnp.bfloat16)

    launch(0)
    first = spread(tokens, gathered, 0)
    for copy in first:
        copy.start()
    launch(1)
    mine.wait()
    for copy in spread_in(gathered, 0):
        copy.wait_recv()
    normalize(gathered, input_gain)

    pump(0)
    launch(2)
    settle(0)
    ret_width = projected.shape[2]
    for t in range(4):
        projected[t] = (
            times(joined, slice(t * ret_width, (t + 1) * ret_width))
            .astype(jnp.bfloat16)
            .astype(jnp.float32)
        )
    pump(1)
    launch(3)

    head_count = rate_ahead.shape[0]
    head_dim = ret_width // head_count
    lane = lax.broadcasted_iota(jnp.int32, (length, ret_width), 1)
    in_lower = lax.rem(lane, head_dim) < head_dim // 2

    def turned(values):
        partner = jnp.where(
            in_lower,
            pltpu.roll(values, ret_width - head_dim // 2, 1),
            pltpu.roll(values, head_dim // 2, 1),
        )
        return values * cosine[...] + partner * sine_part[...]

    queries = turned(projected[0])
    key_heads = (turned(projected[1]) * head_dim ** (-0.5)).astype(jnp.bfloat16)
    valued = projected[2]
    offset = (
        lax.broadcasted_iota(jnp.int32, (length, length), 0)
        - lax.broadcasted_iota(jnp.int32, (length, length), 1)
    ).astype(jnp.float32)
    result = jnp.zeros((length, ret_width), jnp.float32)
    for h in range(head_count):
        here = (lane >= h * head_dim) & (lane < (h + 1) * head_dim)
        scores = lax.dot_general(
            jnp.where(here, queries, 0.0).astype(jnp.bfloat16),
            key_heads,
            (((1,), (1,)), ((), ())),
            preferred_element_type=jnp.float32,
        )
        decay = jnp.exp(jnp.where(offset >= 0, rate_ahead[h] * offset, -rate_behind[h] * offset))
        result = result + jnp.dot(
            (scores * decay).astype(jnp.bfloat16),
            jnp.where(here, valued, 0.0).astype(jnp.bfloat16),
            preferred_element_type=jnp.float32,
        )
    center = jnp.zeros((length, ret_width), jnp.float32)
    for h in range(head_count):
        here = (lane >= h * head_dim) & (lane < (h + 1) * head_dim)
        mean = jnp.sum(jnp.where(here, result, 0.0), axis=1, keepdims=True) / head_dim
        center = jnp.where(here, mean, center)
    centered = result - center
    squared = centered * centered
    factor = jnp.zeros((length, ret_width), jnp.float32)
    for h in range(head_count):
        here = (lane >= h * head_dim) & (lane < (h + 1) * head_dim)
        spread_h = jnp.sum(jnp.where(here, squared, 0.0), axis=1, keepdims=True) / head_dim
        factor = jnp.where(here, lax.rsqrt(spread_h + group_eps), factor)
    gates = projected[3]
    mixed[...] = (gates / (1.0 + jnp.exp(-gates)) * (centered * factor)).astype(jnp.bfloat16)

    settle(1)
    shares(mixed, merge, partial)
    for other in range(1, row):
        scatter(partial, received, 1, other).start()
    total = tokens[...].astype(jnp.float32) + partial[seat].astype(jnp.float32)
    for other in range(1, row):
        scatter(partial, received, 1, other).wait_recv()
        total = total + received[other - 1].astype(jnp.float32)
    gathered_mid[seat] = total.astype(jnp.bfloat16)
    second = spread(gathered_mid.at[seat], gathered_mid, 2)
    for copy in second:
        copy.start()
    pump(2)
    launch(4)
    for copy in spread_in(gathered_mid, 2):
        copy.wait_recv()
    normalize(gathered_mid, middle_gain)
    pump(3)
    settle(2)
    settle(3)
    hidden_width = hidden.shape[1]
    tile = 256 if hidden_width % 256 == 0 else 128

    @pl.loop(0, hidden_width // tile)
    def _(index):
        columns = pl.ds(pl.multiple_of(index * tile, tile), tile)
        gate_act = times(gate, columns)
        up_act = times(up, columns)
        hidden[:, columns] = (gate_act / (1.0 + jnp.exp(-gate_act)) * up_act).astype(jnp.bfloat16)

    pump(4)
    settle(4)
    shares(hidden, down, partial_end)
    for other in range(1, row):
        scatter(partial_end, received_end, 3, other).start()
    total = gathered_mid[seat].astype(jnp.float32) + partial_end[seat].astype(jnp.float32)
    for other in range(1, row):
        scatter(partial_end, received_end, 3, other).wait_recv()
        total = total + received_end[other - 1].astype(jnp.float32)
    out[...] = total.astype(jnp.bfloat16)
    for copy in first + second:
        copy.wait_send()
    for other in range(1, row):
        scatter(partial, received, 1, other).wait_send()
        scatter(partial_end, received_end, 3, other).wait_send()
    for k in range(count):
        drain(k)


def on_device(
    sizes,
    tokens,
    input_gain,
    query_weight,
    key_weight,
    value_weight,
    output_gate_matrix,
    forward_decay,
    backward_decay,
    merge_weight,
    middle_gain,
    gate_weight,
    up_weight,
    down_weight,
):
    seq_count, length, part_width = tokens.shape
    flat = tokens.reshape(seq_count * length, part_width)
    joined = jnp.concatenate([query_weight, key_weight, value_weight, output_gate_matrix], axis=1)
    shards = (joined, merge_weight, gate_weight, up_weight, down_weight)
    line, copies, row, count = sizes["fs"], sizes["grp"], sizes["tp"], len(shards)
    width, ret_width, hidden_width = row * part_width, query_weight.shape[1], gate_weight.shape[1]
    head_count = forward_decay.shape[0]
    tables = turn_tables(length, ret_width // head_count, head_count)
    in_vmem = pl.BlockSpec(memory_space=pltpu.VMEM)
    in_smem = pl.BlockSpec(memory_space=pltpu.SMEM)
    bf16 = jnp.bfloat16
    layer_out = pl.pallas_call(
        functools.partial(layer_kernel, sizes),
        out_shape=jax.ShapeDtypeStruct(flat.shape, bf16),
        in_specs=[in_vmem] * 3
        + [in_smem] * 2
        + [in_vmem] * 2
        + [pl.BlockSpec(memory_space=pl.ANY)] * count,
        out_specs=in_vmem,
        scratch_shapes=[pltpu.VMEM((line,) + w.shape, w.dtype) for w in shards]
        + [
            pltpu.VMEM((row, length, part_width), bf16),
            pltpu.VMEM((row, length, part_width), bf16),
            pltpu.VMEM((length, width), bf16),
            pltpu.VMEM((4, length, ret_width), jnp.float32),
            pltpu.VMEM((length, ret_width), bf16),
            pltpu.VMEM((length, hidden_width), bf16),
            pltpu.VMEM((row, length, part_width), bf16),
            pltpu.VMEM((row - 1, length, part_width), bf16),
            pltpu.VMEM((row, length, part_width), bf16),
            pltpu.VMEM((row - 1, length, part_width), bf16),
            pltpu.SemaphoreType.DMA((count,)),
            pltpu.SemaphoreType.DMA((count, 2, line)),
            pltpu.SemaphoreType.DMA((count, 2, line)),
            pltpu.SemaphoreType.DMA((count, 2, line, copies - 1)),
            pltpu.SemaphoreType.DMA((count, 2, line, copies - 1)),
            pltpu.SemaphoreType.DMA((4, row - 1)),
            pltpu.SemaphoreType.DMA((4, row - 1)),
            pltpu.SemaphoreType.DMA,
        ],
        compiler_params=pltpu.CompilerParams(
            collective_id=0, has_side_effects=True, vmem_limit_bytes=58 << 20
        ),
    )(
        flat,
        input_gain[None, :],
        middle_gain[None, :],
        jax.nn.log_sigmoid(forward_decay),
        jax.nn.log_sigmoid(backward_decay),
        *tables,
        *shards,
    )
    return layer_out.reshape(seq_count, length, part_width)


def solution(mesh):
    placed = (
        P(("grp", "fs"), None, "tp"),
        P(),
        P("fs", "tp"),
        P("fs", "tp"),
        P("fs", "tp"),
        P("fs", "tp"),
        P("tp"),
        P("tp"),
        P("tp", "fs"),
        P(),
        P("fs", "tp"),
        P("fs", "tp"),
        P("tp", "fs"),
    )
    return jax.shard_map(
        functools.partial(on_device, dict(mesh.shape)),
        mesh=mesh,
        in_specs=placed,
        out_specs=P(("grp", "fs"), None, "tp"),
        check_vma=False,
    )
```

```python
import functools

import jax
import jax.numpy as jnp
import numpy as np
from jax import lax
from jax.experimental import pallas as pl
from jax.experimental.pallas import tpu as pltpu
from jax.sharding import PartitionSpec as P

norm_eps = 1e-06
group_eps = 1e-05
rope_base = 10000.0


def turn_tables(length, head_dim, head_count):
    half_dim = head_dim // 2
    inverse = rope_base ** (-np.arange(half_dim) / half_dim)
    angles = np.arange(length)[:, None] * inverse[None, :]
    cosine, sine_part = np.cos(angles), np.sin(angles)
    return (
        np.tile(np.concatenate([cosine, cosine], axis=1), (1, head_count)).astype(np.float32),
        np.tile(np.concatenate([-sine_part, sine_part], axis=1), (1, head_count)).astype(np.float32),
    )


MESH = pl.DeviceIdType.MESH


def layer_kernel(
    sizes,
    tokens,
    input_gain,
    middle_gain,
    rate_ahead,
    rate_behind,
    cosine,
    sine_part,
    joined_shard,
    merge_shard,
    gate_shard,
    up_shard,
    down_shard,
    out,
    joined,
    merge,
    gate,
    up,
    *rest,
):
    line, copies, row = sizes["fs"], sizes["grp"], sizes["tp"]
    parts = len(rest) - 18
    downs, partial_ends, received_ends = rest[:parts], rest[-2], rest[-1]
    (
        gathered,
        gathered_mid,
        normed,
        projected,
        mixed,
        hidden,
        partial,
        received,
        own_sem,
        line_send,
        line_recv,
        pair_send,
        pair_recv,
        row_send,
        row_recv,
        self_sem,
    ) = rest[parts:-2]
    piece_width = downs[0].shape[2]
    shards = (joined_shard, merge_shard, gate_shard, up_shard) + tuple(
        down_shard if parts == 1 else down_shard.at[:, pl.ds(i * piece_width, piece_width)]
        for i in range(parts)
    )
    slots = (joined, merge, gate, up) + tuple(downs)
    count = len(slots)
    length, part_width = tokens.shape
    width = row * part_width
    seat = lax.axis_index("tp")
    place = lax.axis_index("fs")
    half = lax.axis_index("grp")

    barrier = pltpu.get_barrier_semaphore()
    for shift in (1, -1):
        there = place + shift

        @pl.when((there >= 0) & (there < line))
        def _():
            pl.semaphore_signal(barrier, inc=1, device_id={"fs": there}, device_id_type=MESH)

    for other in range(1, copies):
        pl.semaphore_signal(
            barrier,
            inc=1,
            device_id={"grp": lax.rem(half + other, copies)},
            device_id_type=MESH,
        )
    for other in range(1, row):
        pl.semaphore_signal(
            barrier,
            inc=1,
            device_id={"tp": lax.rem(seat + other, row)},
            device_id_type=MESH,
        )
    own = [pltpu.make_async_copy(shards[k], slots[k].at[place], own_sem.at[k]) for k in range(count)]
    for copy in own:
        copy.start()
    neighbours = (place > 0).astype(jnp.int32) + (place < line - 1).astype(jnp.int32)
    mine = pltpu.make_async_copy(tokens, gathered.at[seat], self_sem)
    mine.start()
    pl.semaphore_wait(barrier, neighbours + copies - 1 + row - 1)

    def piece(k, block, part):
        rows = slots[k].shape[1] // copies
        return slots[k].at[block, pl.ds(pl.multiple_of(part * rows, rows), rows), :]

    def hop(k, way, step):
        shift = 1 if way == 0 else -1
        block = place - shift * step
        return pltpu.make_async_remote_copy(
            src_ref=piece(k, block, half),
            dst_ref=piece(k, block, half),
            send_sem=line_send.at[k, way, step],
            recv_sem=line_recv.at[k, way, step],
            device_id={"fs": place + shift},
            device_id_type=MESH,
        )

    def arrival(k, way, step):
        shift = 1 if way == 0 else -1
        block = place - shift * step
        return pltpu.make_async_remote_copy(
            src_ref=piece(k, block, half),
            dst_ref=piece(k, block, half),
            send_sem=line_send.at[k, way, step - 1],
            recv_sem=line_recv.at[k, way, step - 1],
            device_id={"fs": place - shift},
            device_id_type=MESH,
        )

    def across(k, way, step, other):
        shift = 1 if way == 0 else -1
        block = place - shift * step
        return pltpu.make_async_remote_copy(
            src_ref=piece(k, block, half),
            dst_ref=piece(k, block, half),
            send_sem=pair_send.at[k, way, step - 1, other - 1],
            recv_sem=pair_recv.at[k, way, step - 1, other - 1],
            device_id={"grp": lax.rem(half + other, copies)},
            device_id_type=MESH,
        )

    def landed(k, way, step, other):
        shift = 1 if way == 0 else -1
        block = place - shift * step
        source = lax.rem(half + copies - other, copies)
        return pltpu.make_async_remote_copy(
            src_ref=piece(k, block, source),
            dst_ref=piece(k, block, source),
            send_sem=pair_send.at[k, way, step - 1, other - 1],
            recv_sem=pair_recv.at[k, way, step - 1, other - 1],
            device_id={"grp": source},
            device_id_type=MESH,
        )

    def has(way, step):
        return place >= step if way == 0 else place + step < line

    def goes(way):
        return place < line - 1 if way == 0 else place > 0

    def launch(k):
        own[k].wait()
        for way in range(2):

            @pl.when(goes(way))
            def _():
                hop(k, way, 0).start()

    def pump(k):
        for step in range(1, line):
            for way in range(2):

                @pl.when(has(way, step))
                def _():
                    arrival(k, way, step).wait_recv()
                    for other in range(1, copies):
                        across(k, way, step, other).start()

                @pl.when(has(way, step) & goes(way))
                def _():
                    hop(k, way, step).start()

    def settle(k):
        for step in range(1, line):
            for way in range(2):

                @pl.when(has(way, step))
                def _():
                    for other in range(1, copies):
                        landed(k, way, step, other).wait_recv()

    def drain(k):
        for way in range(2):
            for step in range(line):

                @pl.when((has(way, step) if step else True) & goes(way))
                def _():
                    hop(k, way, step).wait_send()

                if step:

                    @pl.when(has(way, step))
                    def _():
                        for other in range(1, copies):
                            across(k, way, step, other).wait_send()

    def spread(source, target, stage):
        return [
            pltpu.make_async_remote_copy(
                src_ref=source,
                dst_ref=target.at[seat],
                send_sem=row_send.at[stage, other - 1],
                recv_sem=row_recv.at[stage, other - 1],
                device_id={"tp": lax.rem(seat + other, row)},
                device_id_type=MESH,
            )
            for other in range(1, row)
        ]

    def spread_in(target, stage):
        sources = [lax.rem(seat + row - other, row) for other in range(1, row)]
        return [
            pltpu.make_async_remote_copy(
                src_ref=target.at[source],
                dst_ref=target.at[source],
                send_sem=row_send.at[stage, other],
                recv_sem=row_recv.at[stage, other],
                device_id={"tp": source},
                device_id_type=MESH,
            )
            for other, source in enumerate(sources)
        ]

    def scatter(source, target, stage, other):
        there = lax.rem(seat + other, row)
        return pltpu.make_async_remote_copy(
            src_ref=source.at[there],
            dst_ref=target.at[other - 1],
            send_sem=row_send.at[stage, other - 1],
            recv_sem=row_recv.at[stage, other - 1],
            device_id={"tp": there},
            device_id_type=MESH,
        )

    def normalize(source, gain_vector):
        total = jnp.zeros((length, 1), jnp.float32)
        for t in range(row):
            widened = source[t].astype(jnp.float32)
            total = total + jnp.sum(widened * widened, axis=1, keepdims=True)
        scale = lax.rsqrt(total / width + norm_eps)
        for t in range(row):
            span = slice(t * part_width, (t + 1) * part_width)
            scaled = source[t].astype(jnp.float32) * scale * gain_vector[:, span]
            normed[:, span] = scaled.astype(jnp.bfloat16)

    def times(weight, columns):
        block = weight[:, :, columns]
        return jnp.dot(
            normed[...], block.reshape(-1, block.shape[2]), preferred_element_type=jnp.float32
        )

    def shares(rows_in, weight, target):
        step = weight.shape[2]
        for block in range(line):
            term = jnp.dot(rows_in[...], weight[block], preferred_element_type=jnp.float32)
            begin = block * step
            inner = begin % part_width
            target[begin // part_width, :, inner : inner + step] = term.astype(jnp.bfloat16)

    def finish(i):
        settle(4 + i)
        if parts == 1:
            shares(hidden, downs[i], partial_ends.at[i])
        else:
            for j in range(row):
                blocks = [jnp.dot(
                    hidden[...], downs[i][j * line // row + c], preferred_element_type=jnp.float32
                ) for c in range(max(1, line // row))]
                for c, term in enumerate(blocks):
                    partial_ends[i, j, :, c * piece_width : (c + 1) * piece_width] = term.astype(
                        jnp.bfloat16
                    )
        for other in range(1, row):
            scatter(partial_ends.at[i], received_ends.at[i], 3 + i, other).start()

    def collect(i):
        span = slice(None) if parts == 1 else slice(i * piece_width, (i + 1) * piece_width)
        total = gathered_mid[seat, :, span].astype(jnp.float32)
        total = total + partial_ends[i, seat].astype(jnp.float32)
        for other in range(1, row):
            scatter(partial_ends.at[i], received_ends.at[i], 3 + i, other).wait_recv()
            total = total + received_ends[i, other - 1].astype(jnp.float32)
        out[:, span] = total.astype(jnp.bfloat16)

    launch(0)
    first = spread(tokens, gathered, 0)
    for copy in first:
        copy.start()
    launch(1)
    mine.wait()
    for copy in spread_in(gathered, 0):
        copy.wait_recv()
    normalize(gathered, input_gain)

    pump(0)
    launch(2)
    settle(0)
    ret_width = projected.shape[2]
    for t in range(4):
        projected[t] = (
            times(joined, slice(t * ret_width, (t + 1) * ret_width))
            .astype(jnp.bfloat16)
            .astype(jnp.float32)
        )
    pump(1)
    launch(3)

    head_count = rate_ahead.shape[0]
    head_dim = ret_width // head_count
    lane = lax.broadcasted_iota(jnp.int32, (length, ret_width), 1)
    in_lower = lax.rem(lane, head_dim) < head_dim // 2

    def turned(values):
        partner = jnp.where(
            in_lower,
            pltpu.roll(values, ret_width - head_dim // 2, 1),
            pltpu.roll(values, head_dim // 2, 1),
        )
        return values * cosine[...] + partner * sine_part[...]

    queries = turned(projected[0])
    key_heads = (turned(projected[1]) * head_dim ** (-0.5)).astype(jnp.bfloat16)
    valued = projected[2]
    offset = (
        lax.broadcasted_iota(jnp.int32, (length, length), 0)
        - lax.broadcasted_iota(jnp.int32, (length, length), 1)
    ).astype(jnp.float32)
    result = jnp.zeros((length, ret_width), jnp.float32)
    for h in range(head_count):
        here = (lane >= h * head_dim) & (lane < (h + 1) * head_dim)
        scores = lax.dot_general(
            jnp.where(here, queries, 0.0).astype(jnp.bfloat16),
            key_heads,
            (((1,), (1,)), ((), ())),
            preferred_element_type=jnp.float32,
        )
        decay = jnp.exp(jnp.where(offset >= 0, rate_ahead[h] * offset, -rate_behind[h] * offset))
        result = result + jnp.dot(
            (scores * decay).astype(jnp.bfloat16),
            jnp.where(here, valued, 0.0).astype(jnp.bfloat16),
            preferred_element_type=jnp.float32,
        )
    center = jnp.zeros((length, ret_width), jnp.float32)
    for h in range(head_count):
        here = (lane >= h * head_dim) & (lane < (h + 1) * head_dim)
        mean = jnp.sum(jnp.where(here, result, 0.0), axis=1, keepdims=True) / head_dim
        center = jnp.where(here, mean, center)
    centered = result - center
    squared = centered * centered
    factor = jnp.zeros((length, ret_width), jnp.float32)
    for h in range(head_count):
        here = (lane >= h * head_dim) & (lane < (h + 1) * head_dim)
        spread_h = jnp.sum(jnp.where(here, squared, 0.0), axis=1, keepdims=True) / head_dim
        factor = jnp.where(here, lax.rsqrt(spread_h + group_eps), factor)
    gates = projected[3]
    mixed[...] = (gates / (1.0 + jnp.exp(-gates)) * (centered * factor)).astype(jnp.bfloat16)

    settle(1)
    shares(mixed, merge, partial)
    for other in range(1, row):
        scatter(partial, received, 1, other).start()
    pump(2)
    total = tokens[...].astype(jnp.float32) + partial[seat].astype(jnp.float32)
    for other in range(1, row):
        scatter(partial, received, 1, other).wait_recv()
        total = total + received[other - 1].astype(jnp.float32)
    gathered_mid[seat] = total.astype(jnp.bfloat16)
    second = spread(gathered_mid.at[seat], gathered_mid, 2)
    for copy in second:
        copy.start()
    pump(3)
    launch(4)
    if parts > 1:
        launch(5)
    for copy in spread_in(gathered_mid, 2):
        copy.wait_recv()
    normalize(gathered_mid, middle_gain)
    settle(2)
    settle(3)
    hidden_width = hidden.shape[1]
    tile = 256 if hidden_width % 256 == 0 else 128

    @pl.loop(0, hidden_width // tile)
    def _(index):
        columns = pl.ds(pl.multiple_of(index * tile, tile), tile)
        gate_act = times(gate, columns)
        up_act = times(up, columns)
        hidden[:, columns] = (gate_act / (1.0 + jnp.exp(-gate_act)) * up_act).astype(jnp.bfloat16)

    for i in range(parts):
        pump(4 + i)
        if i + 2 < parts:
            launch(6 + i)
        if i:
            finish(i - 1)
    finish(parts - 1)
    for i in range(parts):
        collect(i)
    for copy in first + second:
        copy.wait_send()
    for other in range(1, row):
        scatter(partial, received, 1, other).wait_send()
        for i in range(parts):
            scatter(partial_ends.at[i], received_ends.at[i], 3 + i, other).wait_send()
    for k in range(count):
        drain(k)


def on_device(
    sizes,
    tokens,
    input_gain,
    query_weight,
    key_weight,
    value_weight,
    output_gate_matrix,
    forward_decay,
    backward_decay,
    merge_weight,
    middle_gain,
    gate_weight,
    up_weight,
    down_weight,
):
    seq_count, length, part_width = tokens.shape
    flat = tokens.reshape(seq_count * length, part_width)
    joined = jnp.concatenate([query_weight, key_weight, value_weight, output_gate_matrix], axis=1)
    shards = (joined, merge_weight, gate_weight, up_weight, down_weight)
    line, copies, row = sizes["fs"], sizes["grp"], sizes["tp"]
    down_width = down_weight.shape[1]
    parts = down_width // 256 if line == row and down_width % 256 == 0 else 1
    down_piece = jax.ShapeDtypeStruct((down_weight.shape[0], down_width // parts), jnp.bfloat16)
    landing = shards[:4] + (down_piece,) * parts
    count = len(landing)
    width, ret_width, hidden_width = row * part_width, query_weight.shape[1], gate_weight.shape[1]
    head_count = forward_decay.shape[0]
    tables = turn_tables(length, ret_width // head_count, head_count)
    in_vmem = pl.BlockSpec(memory_space=pltpu.VMEM)
    in_smem = pl.BlockSpec(memory_space=pltpu.SMEM)
    bf16 = jnp.bfloat16
    layer_out = pl.pallas_call(
        functools.partial(layer_kernel, sizes),
        out_shape=jax.ShapeDtypeStruct(flat.shape, bf16),
        in_specs=[in_vmem] * 3
        + [in_smem] * 2
        + [in_vmem] * 2
        + [pl.BlockSpec(memory_space=pl.ANY)] * len(shards),
        out_specs=in_vmem,
        scratch_shapes=[pltpu.VMEM((line,) + w.shape, w.dtype) for w in landing]
        + [
            pltpu.VMEM((row, length, part_width), bf16),
            pltpu.VMEM((row, length, part_width), bf16),
            pltpu.VMEM((length, width), bf16),
            pltpu.VMEM((4, length, ret_width), jnp.float32),
            pltpu.VMEM((length, ret_width), bf16),
            pltpu.VMEM((length, hidden_width), bf16),
            pltpu.VMEM((row, length, part_width), bf16),
            pltpu.VMEM((row - 1, length, part_width), bf16),
            pltpu.SemaphoreType.DMA((count,)),
            pltpu.SemaphoreType.DMA((count, 2, line)),
            pltpu.SemaphoreType.DMA((count, 2, line)),
            pltpu.SemaphoreType.DMA((count, 2, line, copies - 1)),
            pltpu.SemaphoreType.DMA((count, 2, line, copies - 1)),
            pltpu.SemaphoreType.DMA((3 + parts, row - 1)),
            pltpu.SemaphoreType.DMA((3 + parts, row - 1)),
            pltpu.SemaphoreType.DMA,
            pltpu.VMEM((parts, row, length, part_width // parts), bf16),
            pltpu.VMEM((parts, row - 1, length, part_width // parts), bf16),
        ],
        compiler_params=pltpu.CompilerParams(
            collective_id=0, has_side_effects=True, vmem_limit_bytes=58 << 20
        ),
    )(
        flat,
        input_gain[None, :],
        middle_gain[None, :],
        jax.nn.log_sigmoid(forward_decay),
        jax.nn.log_sigmoid(backward_decay),
        *tables,
        *shards,
    )
    return layer_out.reshape(seq_count, length, part_width)


def solution(mesh):
    placed = (
        P(("grp", "fs"), None, "tp"),
        P(),
        P("fs", "tp"),
        P("fs", "tp"),
        P("fs", "tp"),
        P("fs", "tp"),
        P("tp"),
        P("tp"),
        P("tp", "fs"),
        P(),
        P("fs", "tp"),
        P("fs", "tp"),
        P("tp", "fs"),
    )
    return jax.shard_map(
        functools.partial(on_device, dict(mesh.shape)),
        mesh=mesh,
        in_specs=placed,
        out_specs=P(("grp", "fs"), None, "tp"),
        check_vma=False,
    )
```
